32 devices in a mesh: ep: 16 (over z, y, x), tp: 2 (over core).
Axes of the slice: x: 2, y: 2, z: 4, core: 2. Of those that a mesh axis runs over, the one named last changes fastest.
Arguments:
- tokens: bfloat16 [64, 4096], P('ep'), may hold values from -6 to 6
- memory: float32 [64, 8, 256, 512], P('ep', 'tp'), may hold values from -6 to 6
- normalizer: float32 [64, 8, 256], P('ep', 'tp'), may hold values from -6 to 6
- stabilizer: float32 [64, 8], P('ep', 'tp'), may hold values from -4 to 4
- norm_gain: float32 [4096], replicated, may hold values from 0.1 to 1.9
- w_query: bfloat16 [4096, 8, 256], P(None, 'tp', 'ep'), may hold values from -0.09375 to 0.09375
- w_key: bfloat16 [4096, 8, 256], P(None, 'tp', 'ep'), may hold values from -0.09375 to 0.09375
- w_value: bfloat16 [4096, 8, 512], P(None, 'tp', 'ep'), may hold values from -0.09375 to 0.09375
- w_outgate: bfloat16 [4096, 8, 512], P(None, 'tp', 'ep'), may hold values from -0.09375 to 0.09375
- w_input: bfloat16 [4096, 8], P(None, 'tp'), may hold values from -0.09375 to 0.09375
- w_forget: bfloat16 [4096, 8], P(None, 'tp'), may hold values from -0.09375 to 0.09375
- forget_bias: float32 [8], P('tp'), may hold values from 0 to 4
- w_out: bfloat16 [4096, 4096], P('tp', 'ep'), may hold values from -0.09375 to 0.09375
- ffn_gain: float32 [4096], replicated, may hold values from 0.1 to 1.9
- w_gate: bfloat16 [16, 4096, 512], P('ep', None, 'tp'), may hold values from -0.09375 to 0.09375
- w_up: bfloat16 [16, 4096, 512], P('ep', None, 'tp'), may hold values from -0.09375 to 0.09375
- w_down: bfloat16 [16, 512, 4096], P('ep', 'tp'), may hold values from -0.25 to 0.25
- expert_ids: int32 [64, 2], P('ep'), may hold values from 0 to 15, as said below
- route_weights: float32 [64, 2], P('ep'), may hold values from 0.1 to 1
Outputs:
- out: bfloat16 [64, 4096], P('ep')
- memory_next: float32 [64, 8, 256, 512], P('ep', 'tp')
- normalizer_next: float32 [64, 8, 256], P('ep', 'tp')
- stabilizer_next: float32 [64, 8], P('ep', 'tp')
The draws below stay inside these ranges and needn't reach their ends.
Inputs may be any that keep to these rules, and one draw needn't show every extreme that they name: `expert_ids`: the 2 experts of a token differ and lie in one group of 8 consecutive experts. Beyond that, any choice is allowed: for instance, all 4 tokens of one index of ep may name the same expert.
All inputs are finite; a program needn't handle non-finite values.
Results may differ from the reference program's by a relative error of at most 0.013.
Values may be sent and summed in bfloat16 or wider, within the bound.
A program may use at most 128 MiB of HBM per device.

```python
import jax
import jax.numpy as jnp
from jax import lax

D = 4096
HEADS = 8
DK = 256
DV = 512
DFF = 512
EXPERTS_PER_GROUP = 8
TOP = 2
SEQ_DEV = 4
SEQS = 64
EXPERTS = 16
GROUPS = 2
N_TP = 2


def draw_expert_ids(key, part):
    keys = jax.random.split(jax.random.fold_in(key, 7), 5)
    owner = jnp.arange(SEQS) // SEQ_DEV
    groups = jnp.minimum(jax.random.randint(keys[0], (SEQS,), 0, GROUPS), jax.random.randint(keys[1], (SEQS,), 0, GROUPS))
    first = jax.random.randint(keys[2], (SEQS,), 0, EXPERTS_PER_GROUP)
    offset = jax.random.randint(keys[3], (SEQS,), 1, EXPERTS_PER_GROUP)
    chosen = jax.random.randint(keys[4], (), 0, SEQS // SEQ_DEV)
    leader = chosen * SEQ_DEV
    groups = jnp.where(owner == chosen, groups[leader], groups)
    first = jnp.where(owner == chosen, first[leader], first)
    second = (first + offset) % EXPERTS_PER_GROUP
    return jnp.stack([groups * EXPERTS_PER_GROUP + first, groups * EXPERTS_PER_GROUP + second], axis=1).astype(jnp.int32)


def level_of(stream_key, shape, shards, least, high):
    def one(axis_at, blocks):
        heights = jax.random.uniform(jax.random.fold_in(jax.random.fold_in(stream_key, 6), axis_at), (blocks,), jnp.float32, least / len(shards), high / len(shards))
        return jnp.repeat(jnp.exp(heights), shape[axis_at] // blocks).reshape((-1,) + (1,) * (len(shape) - axis_at - 1))

    factor_of = one(*shards[0])
    for cut in shards[1:]:
        factor_of = factor_of * one(*cut)
    return factor_of


def gaussian(stream_key, shape, scale, most, cuts=(), held_as=jnp.bfloat16):
    entries = scale * jax.random.normal(stream_key, shape, jnp.float32)
    if cuts:
        entries = entries * level_of(stream_key, shape, cuts, -0.22, 0.18)
    return jnp.clip(entries, -most, most).astype(held_as)


def setup_inputs(seed: int = 0) -> dict:
    arg_keys = jax.random.split(jax.random.key(seed), 20)
    return {
        "tokens": gaussian(arg_keys[0], (SEQS, D), 1.0, 6.0, ((0, 16),)),
        "memory": gaussian(arg_keys[1], (SEQS, HEADS, DK, DV), 1.0, 6.0, ((0, 16), (1, 2)), jnp.float32),
        "normalizer": gaussian(arg_keys[2], (SEQS, HEADS, DK), 1.0, 6.0, ((0, 16), (1, 2)), jnp.float32),
        "stabilizer": gaussian(arg_keys[3], (SEQS, HEADS), 1.0, 4.0, ((0, 16), (1, 2)), jnp.float32),
        "norm_gain": jnp.clip(1.0 + 0.18 * jax.random.normal(arg_keys[4], (D,), jnp.float32), 0.1, 1.9),
        "w_query": gaussian(arg_keys[5], (D, HEADS, DK), D ** -0.5, 0.09375, ((1, 2), (2, 16))),
        "w_key": gaussian(arg_keys[6], (D, HEADS, DK), D ** -0.5, 0.09375, ((1, 2), (2, 16))),
        "w_value": gaussian(arg_keys[7], (D, HEADS, DV), D ** -0.5, 0.09375, ((1, 2), (2, 16))),
        "w_outgate": gaussian(arg_keys[8], (D, HEADS, DV), D ** -0.5, 0.09375, ((1, 2), (2, 16))),
        "w_input": gaussian(arg_keys[9], (D, HEADS), D ** -0.5, 0.09375, ((1, 2),)),
        "w_forget": gaussian(arg_keys[10], (D, HEADS), D ** -0.5, 0.09375, ((1, 2),)),
        "forget_bias": jnp.clip(4.0 * jax.random.uniform(arg_keys[11], (HEADS,), jnp.float32) ** level_of(arg_keys[11], (HEADS,), ((0, 2),), -0.2, 0.2), 0.0, 4.0),
        "w_out": gaussian(arg_keys[12], (HEADS * DV, D), (HEADS * DV) ** -0.5, 0.09375, ((0, 2), (1, 16))),
        "ffn_gain": jnp.clip(1.0 + 0.18 * jax.random.normal(arg_keys[13], (D,), jnp.float32), 0.1, 1.9),
        "w_gate": gaussian(arg_keys[14], (EXPERTS, D, DFF), D ** -0.5, 0.09375, ((0, 16), (2, 2))),
        "w_up": gaussian(arg_keys[15], (EXPERTS, D, DFF), D ** -0.5, 0.09375, ((0, 16), (2, 2))),
        "w_down": gaussian(arg_keys[16], (EXPERTS, DFF, D), DFF ** -0.5, 0.25, ((0, 16), (1, 2))),
        "expert_ids": draw_expert_ids(jax.random.fold_in(arg_keys[19], 71), 0),
        "route_weights": jnp.clip(0.1 + 0.9 * jax.random.uniform(arg_keys[18], (SEQS, TOP), jnp.float32) ** level_of(arg_keys[18], (SEQS, TOP), ((0, 16),), -0.2, 0.2), 0.1, 1.0),
    }


def rms_scale(values, gain):
    return values * lax.rsqrt(lax.optimization_barrier(jnp.mean(values * values, axis=-1, keepdims=True)) + 1e-06) * gain

def product(left, right):
    return jnp.dot(left, right, preferred_element_type=jnp.float32)

def rounded_term(values):
    return lax.optimization_barrier(values.astype(jnp.bfloat16)).astype(jnp.float32)

def cell_step(inputs):
    memory, normalizer, stabilizer, scaled, key, value, in_pre, log_forget = inputs
    stab_next = jnp.maximum(log_forget + stabilizer, in_pre)
    decay = jnp.exp(log_forget + stabilizer - stab_next)
    inweight = jnp.exp(in_pre - stab_next)
    memory_next = decay[:, None, None] * memory + inweight[:, None, None] * (key[:, :, None] * value[:, None, :])
    normalizer_next = decay[:, None] * normalizer + inweight[:, None] * key
    numerator = jnp.einsum('hd,hde->he', scaled, memory_next, precision=lax.Precision.HIGHEST)
    denominator = lax.optimization_barrier(jnp.sum(scaled * normalizer_next, axis=-1))
    hidden = numerator / jnp.maximum(jnp.abs(denominator), jnp.exp(-stab_next))[:, None]
    return (memory_next, normalizer_next, stab_next, hidden)

def reference(tokens, memory, normalizer, stabilizer, norm_gain, w_query, w_key, w_value, w_outgate, w_input, w_forget, forget_bias, w_out, ffn_gain, w_gate, w_up, w_down, expert_ids, route_weights):
    seqs = tokens.shape[0]
    normed = rms_scale(tokens.astype(jnp.float32), norm_gain).astype(jnp.bfloat16)
    query = product(normed, w_query.reshape(D, HEADS * DK)).astype(jnp.bfloat16)
    key = product(normed, w_key.reshape(D, HEADS * DK)).astype(jnp.bfloat16)
    value = product(normed, w_value.reshape(D, HEADS * DV)).astype(jnp.bfloat16)
    outgate = product(normed, w_outgate.reshape(D, HEADS * DV)).astype(jnp.bfloat16)
    in_pre = product(normed, w_input)
    log_forget = jax.nn.log_sigmoid(product(normed, w_forget) + forget_bias)
    scaled = query.astype(jnp.float32).reshape(seqs, HEADS, DK) * DK ** (-0.5)
    key_heads = key.astype(jnp.float32).reshape(seqs, HEADS, DK)
    value_heads = value.astype(jnp.float32).reshape(seqs, HEADS, DV)
    memory_next, normalizer_next, stab_next, hidden = lax.map(cell_step, (memory, normalizer, stabilizer, scaled, key_heads, value_heads, in_pre, log_forget))
    hidden = (hidden.reshape(seqs, HEADS * DV) * jax.nn.sigmoid(outgate.astype(jnp.float32))).astype(jnp.bfloat16)
    span = HEADS * DV // N_TP
    mixed = jnp.zeros((seqs, D), jnp.float32)
    for member in range(N_TP):
        mixed = mixed + rounded_term(product(hidden[:, member * span:(member + 1) * span], w_out[member * span:(member + 1) * span]))
    mixed = mixed.astype(jnp.bfloat16)
    resid = tokens.astype(jnp.float32) + mixed.astype(jnp.float32)
    ffn_in = rms_scale(resid, ffn_gain).astype(jnp.bfloat16)
    hidden_span = DFF // N_TP

    def expert_row(inputs):
        row, expert, weight = inputs
        gate_part = product(row, w_gate[expert])
        up_part = product(row, w_up[expert])
        act = (jax.nn.silu(gate_part) * up_part).astype(jnp.bfloat16)
        down = w_down[expert]
        total = jnp.zeros((D,), jnp.float32)
        for member in range(N_TP):
            total = total + weight * rounded_term(product(act[member * hidden_span:(member + 1) * hidden_span], down[member * hidden_span:(member + 1) * hidden_span]))
        return total
    rows = jnp.repeat(ffn_in, TOP, axis=0)
    weighted = lax.map(expert_row, (rows, expert_ids.reshape(-1).astype(jnp.int32), route_weights.reshape(-1)))
    ffn_out = lax.optimization_barrier(jnp.sum(weighted.reshape(seqs, TOP, D), axis=1))
    out = (resid + ffn_out).astype(jnp.bfloat16)
    return (out, memory_next, normalizer_next, stab_next)
```

```python
import functools

import jax
import jax.numpy as jnp
from jax import lax
from jax.experimental import pallas as pl
from jax.experimental.pallas import tpu as pltpu
from jax.sharding import PartitionSpec as P

MESH = pl.DeviceIdType.MESH
VMEM_LIMIT = 48 * 1024 * 1024


def product(left, right):
    return jnp.dot(left, right, preferred_element_type=jnp.float32)


def product_nt(left, right):
    return lax.dot_general(left, right, (((1,), (1,)), ((), ())), preferred_element_type=jnp.float32)


def rms_scale(values, gain):
    return values * lax.rsqrt(jnp.mean(values * values, axis=-1, keepdims=True) + 1e-06) * gain


def remote(src, dst, send_sem, recv_sem, device):
    return pltpu.make_async_remote_copy(
        src_ref=src, dst_ref=dst, send_sem=send_sem, recv_sem=recv_sem, device_id=device, device_id_type=MESH
    )


def each(low, high, step):
    def run(at, carry):
        step(at)
        return carry

    lax.fori_loop(low, high, run, 0)


def stack_rows(pieces, dest):
    rows = pieces[0]().shape[0]
    group = max(1, 16 // rows)
    for first in range(0, len(pieces), group):
        block = jnp.concatenate([piece() for piece in pieces[first : first + group]], axis=0)
        dest[first * rows : first * rows + block.shape[0], :] = block.astype(jnp.bfloat16)


class HalfGather:
    def __init__(self, n, own, gathered, sems):
        self.n, self.own, self.gathered = n, own, gathered
        self.send, self.recv, self.relay_send, self.relay_recv = sems
        self.me, self.t = lax.axis_index("ep"), lax.axis_index("tp")

    def source(self, d):
        return lax.rem(self.me + self.n - d, self.n)

    def out(self, d):
        return remote(
            self.own.at[self.t],
            self.gathered.at[self.me, self.t],
            self.send.at[d],
            self.recv.at[d],
            (lax.rem(self.me + d, self.n), self.t),
        )

    def arrival(self, d):
        slot = self.gathered.at[self.source(d), self.t]
        return remote(self.own.at[self.t], slot, self.send.at[d], self.recv.at[d], (self.me, 1 - self.t))

    def relay(self, d, half):
        slot = self.gathered.at[self.source(d), half]
        return remote(slot, slot, self.relay_send.at[d], self.relay_recv.at[d], (self.me, 1 - self.t))

    def start(self):
        each(1, self.n, lambda d: self.out(d).start())
        self.gathered[self.me] = self.own[...]

    def finish(self):
        def pass_on(d):
            self.arrival(d).wait_recv()
            self.relay(d, self.t).start()

        each(1, self.n, pass_on)
        each(1, self.n, lambda d: self.relay(d, 1 - self.t).wait_recv())

    def drain(self):
        def step(d):
            self.out(d).wait_send()
            self.relay(d, self.t).wait_send()

        each(1, self.n, step)


class Exchange:
    def __init__(self, n, outbox, inbox, send, recv, broadcast=False):
        self.n, self.outbox, self.inbox, self.send, self.recv = n, outbox, inbox, send, recv
        self.broadcast = broadcast
        self.me, self.t = lax.axis_index("ep"), lax.axis_index("tp")

    def out(self, d):
        to = lax.rem(self.me + d, self.n)
        src = self.outbox if self.broadcast else self.outbox.at[to]
        return remote(src, self.inbox.at[self.me], self.send.at[d], self.recv.at[d], (to, self.t))

    def arrival(self, d):
        source = lax.rem(self.me + self.n - d, self.n)
        src = self.outbox if self.broadcast else self.outbox.at[source]
        return remote(src, self.inbox.at[source], self.send.at[d], self.recv.at[d], (source, self.t))

    def start(self):
        each(1, self.n, lambda d: self.out(d).start())
        self.inbox[self.me] = self.outbox[...] if self.broadcast else self.outbox[self.me]

    def finish(self):
        each(1, self.n, lambda d: self.arrival(d).wait_recv())

    def drain(self):
        each(1, self.n, lambda d: self.out(d).wait_send())


def cell_in_kernel(
    n,
    tokens_ref, gain_ref, win_ref, wforget_ref, wq_ref, wk_ref, wv_ref, wo_ref,
    inpre_ref, fpre_ref, proj_ref,
    own, gathered, weights, rows_lo, rows_hi, outbox, inbox,
    wsem, send, recv, rsend, rrecv, xsend, xrecv,
):
    me, t = lax.axis_index("ep"), lax.axis_index("tp")
    loads, first = [], 0
    for index, ref in enumerate((wq_ref, wk_ref, wv_ref, wo_ref)):
        count = ref.shape[0]
        loads.append(pltpu.make_async_copy(ref, weights.at[pl.ds(first, count)], wsem.at[index]))
        first += count
    for load in loads:
        load.start()
    barrier = pltpu.get_barrier_semaphore()
    each(1, n, lambda d: pl.semaphore_signal(barrier, inc=1, device_id=(lax.rem(me + d, n), t), device_id_type=MESH))
    pl.semaphore_signal(barrier, inc=1, device_id=(me, 1 - t), device_id_type=MESH)

    half = own.shape[2]
    seqs = own.shape[1]
    normed = rms_scale(tokens_ref[...].astype(jnp.float32), gain_ref[...]).astype(jnp.bfloat16)
    own[0] = normed[:, :half]
    own[1] = normed[:, half:]
    pl.semaphore_wait(barrier, n)

    gather = HalfGather(n, own, gathered, (send, recv, rsend, rrecv))
    gather.start()
    inpre_ref[...] = product_nt(normed, win_ref[...])
    fpre_ref[...] = product_nt(normed, wforget_ref[...])
    gather.finish()
    for index, dest in enumerate((rows_lo, rows_hi)):
        stack_rows([functools.partial(lambda p, i: gathered[p, i].astype(jnp.float32), p, index) for p in range(n)], dest)
    for load in loads:
        load.wait()
    result = product_nt(rows_lo[...], weights[:, :half]) + product_nt(rows_hi[...], weights[:, half:])
    for p in range(n):
        outbox[p] = result[p * seqs : (p + 1) * seqs].astype(jnp.bfloat16)
    swap = Exchange(n, outbox, inbox, xsend, xrecv)
    swap.start()
    swap.finish()
    proj_ref[...] = inbox[...]
    gather.drain()
    swap.drain()


def ffn_kernel(
    n,
    hidden_ref, tokens_ref, gain_ref, route_ref, wout_ref, wgate_ref, wup_ref, wdown_ref,
    out_ref,
    heads_in, rows_h, wout, mixbox, mixin, resid, own, gathered, rows_lo, rows_hi,
    wgate, wup, wdown, terms, other, outbox, inbox, halves,
    wsem, hsend, hrecv, msend, mrecv, send, recv, rsend, rrecv, tsend, trecv, xsend, xrecv, osend, orecv,
):
    me, t = lax.axis_index("ep"), lax.axis_index("tp")
    loads = [
        pltpu.make_async_copy(ref, dest, wsem.at[index])
        for index, (ref, dest) in enumerate(((wout_ref, wout), (wgate_ref, wgate), (wup_ref, wup), (wdown_ref, wdown)))
    ]
    for load in loads:
        load.start()
    barrier = pltpu.get_barrier_semaphore()

    def greet(d):
        to = lax.rem(me + d, n)
        pl.semaphore_signal(barrier, inc=1, device_id=(to, t), device_id_type=MESH)
        pl.semaphore_signal(barrier, inc=1, device_id=(to, 1 - t), device_id_type=MESH)

    each(1, n, greet)
    pl.semaphore_signal(barrier, inc=1, device_id=(me, 1 - t), device_id_type=MESH)
    pl.semaphore_wait(barrier, 2 * n - 1)

    seqs, half = own.shape[1], own.shape[2]
    heads = Exchange(n, hidden_ref, heads_in, hsend, hrecv, broadcast=True)
    heads.start()
    heads.finish()
    stack_rows([functools.partial(lambda p: heads_in[p].astype(jnp.float32), p) for p in range(n)], rows_h)
    loads[0].wait()
    partial_value = product(rows_h[...], wout[...])
    for p in range(n):
        mixbox[p] = partial_value[p * seqs : (p + 1) * seqs].astype(jnp.bfloat16)

    def mix_out(d, c):
        to = lax.rem(me + d, n)
        to_t = t if c == 0 else 1 - t
        return remote(mixbox.at[to], mixin.at[t, me], msend.at[c, d], mrecv.at[c, d], (to, to_t))

    def mix_arrival(d, c):
        source = lax.rem(me + n - d, n)
        from_t = t if c == 0 else 1 - t
        return remote(mixbox.at[source], mixin.at[from_t, source], msend.at[c, d], mrecv.at[c, d], (source, 1 - t))

    each(1, n, lambda d: mix_out(d, 0).start())
    each(0, n, lambda d: mix_out(d, 1).start())
    mixin[t, me] = mixbox[me]
    each(1, n, lambda d: mix_arrival(d, 0).wait_recv())
    each(0, n, lambda d: mix_arrival(d, 1).wait_recv())
    piece = mixin.shape[3]
    for p in range(n):
        mixed = (mixin[0, p].astype(jnp.float32) + mixin[1, p].astype(jnp.float32)).astype(jnp.bfloat16)
        columns = slice(p * piece, (p + 1) * piece)
        resid[:, columns] = tokens_ref[:, columns].astype(jnp.float32) + mixed.astype(jnp.float32)
    ffn_in = rms_scale(resid[...], gain_ref[...]).astype(jnp.bfloat16)
    own[0] = ffn_in[:, :half]
    own[1] = ffn_in[:, half:]
    gather = HalfGather(n, own, gathered, (send, recv, rsend, rrecv))
    gather.start()
    gather.finish()
    for index, dest in enumerate((rows_lo, rows_hi)):
        stack_rows([functools.partial(lambda p, i: gathered[p, i].astype(jnp.float32), p, index) for p in range(n)], dest)
    loads[1].wait()
    gate = product(rows_lo[...], wgate[:half]) + product(rows_hi[...], wgate[half:])
    loads[2].wait()
    up = product(rows_lo[...], wup[:half]) + product(rows_hi[...], wup[half:])
    act = (jax.nn.silu(gate) * up).astype(jnp.bfloat16)
    loads[3].wait()
    width = min(512, half)
    for index in range(2):
        for first in range(0, half, width):
            block = product(act, wdown[:, index * half + first : index * half + first + width])
            terms[index, :, first : first + width] = block.astype(jnp.bfloat16)
    across = remote(terms.at[1 - t], other, tsend, trecv, (me, 1 - t))
    across.start()
    across.wait_recv()
    rows = max(seqs, 16)
    for first in range(0, n * seqs, rows):
        both = terms[t, first : first + rows].astype(jnp.float32) + other[first : first + rows].astype(jnp.float32)
        for at in range(rows // seqs):
            outbox[first // seqs + at] = both[at * seqs : (at + 1) * seqs].astype(jnp.bfloat16)
    swap = Exchange(n, outbox, inbox, xsend, xrecv)
    swap.start()
    swap.finish()
    total = route_ref[:, 0:1] * inbox[0].astype(jnp.float32)
    for p in range(1, n):
        total = total + route_ref[:, p : p + 1] * inbox[p].astype(jnp.float32)
    halves[t] = total.astype(jnp.bfloat16)
    give = remote(halves.at[t], halves.at[t], osend, orecv, (me, 1 - t))
    take = remote(halves.at[1 - t], halves.at[1 - t], osend, orecv, (me, 1 - t))
    give.start()
    take.wait_recv()
    for index in range(2):
        columns = slice(index * half, (index + 1) * half)
        out_ref[:, columns] = (resid[:, columns] + halves[index].astype(jnp.float32)).astype(jnp.bfloat16)
    heads.drain()
    each(1, n, lambda d: mix_out(d, 0).wait_send())
    each(0, n, lambda d: mix_out(d, 1).wait_send())
    gather.drain()
    across.wait_send()
    swap.drain()
    give.wait_send()


def vmem_spec():
    return pl.BlockSpec(memory_space=pltpu.VMEM)


def any_spec():
    return pl.BlockSpec(memory_space=pl.ANY)


def cell_in(n, tokens, gain, w_input, w_forget, w_query, w_key, w_value, w_outgate):
    seqs, width = tokens.shape
    flat = [jnp.transpose(w, (1, 2, 0)).reshape(-1, width) for w in (w_query, w_key, w_value, w_outgate)]
    columns = sum(w.shape[0] for w in flat)
    heads = w_input.shape[1]
    bf16 = jnp.bfloat16
    dma = pltpu.SemaphoreType.DMA
    return pl.pallas_call(
        functools.partial(cell_in_kernel, n),
        out_shape=(
            jax.ShapeDtypeStruct((seqs, heads), jnp.float32),
            jax.ShapeDtypeStruct((seqs, heads), jnp.float32),
            jax.ShapeDtypeStruct((n, seqs, columns), bf16),
        ),
        in_specs=[vmem_spec()] * 4 + [any_spec()] * 4,
        out_specs=(vmem_spec(),) * 3,
        scratch_shapes=[
            pltpu.VMEM((2, seqs, width // 2), bf16),
            pltpu.VMEM((n, 2, seqs, width // 2), bf16),
            pltpu.VMEM((columns, width), bf16),
            pltpu.VMEM((n * seqs, width // 2), bf16),
            pltpu.VMEM((n * seqs, width // 2), bf16),
            pltpu.VMEM((n, seqs, columns), bf16),
            pltpu.VMEM((n, seqs, columns), bf16),
            dma((4,)),
        ]
        + [dma((n,))] * 6,
        compiler_params=pltpu.CompilerParams(collective_id=0, has_side_effects=True, vmem_limit_bytes=VMEM_LIMIT),
        name="cell_in",
    )(tokens, gain.reshape(1, width), w_input.T, w_forget.T, *flat)


def ffn(n, hidden, tokens, gain, route, w_out, w_gate, w_up, w_down):
    seqs, width = tokens.shape
    half = width // 2
    bf16 = jnp.bfloat16
    dma = pltpu.SemaphoreType.DMA
    return pl.pallas_call(
        functools.partial(ffn_kernel, n),
        out_shape=jax.ShapeDtypeStruct((seqs, width), bf16),
        in_specs=[vmem_spec()] * 4 + [any_spec()] * 4,
        out_specs=vmem_spec(),
        scratch_shapes=[
            pltpu.VMEM((n, seqs, hidden.shape[1]), bf16),
            pltpu.VMEM((n * seqs, hidden.shape[1]), bf16),
            pltpu.VMEM(w_out.shape, bf16),
            pltpu.VMEM((n, seqs, w_out.shape[1]), bf16),
            pltpu.VMEM((2, n, seqs, w_out.shape[1]), bf16),
            pltpu.VMEM((seqs, width), jnp.float32),
            pltpu.VMEM((2, seqs, half), bf16),
            pltpu.VMEM((n, 2, seqs, half), bf16),
            pltpu.VMEM((n * seqs, half), bf16),
            pltpu.VMEM((n * seqs, half), bf16),
            pltpu.VMEM(w_gate.shape, bf16),
            pltpu.VMEM(w_up.shape, bf16),
            pltpu.VMEM(w_down.shape, bf16),
            pltpu.VMEM((2, n * seqs, half), bf16),
            pltpu.VMEM((n * seqs, half), bf16),
            pltpu.VMEM((n, seqs, half), bf16),
            pltpu.VMEM((n, seqs, half), bf16),
            pltpu.VMEM((2, seqs, half), bf16),
            dma((4,)),
            dma((n,)),
            dma((n,)),
            dma((2, n)),
            dma((2, n)),
            dma((n,)),
            dma((n,)),
            dma((n,)),
            dma((n,)),
            dma,
            dma,
            dma((n,)),
            dma((n,)),
            dma,
            dma,
        ],
        compiler_params=pltpu.CompilerParams(collective_id=1, has_side_effects=True, vmem_limit_bytes=VMEM_LIMIT),
        name="ffn",
    )(hidden, tokens, gain.reshape(1, width), route, w_out, w_gate, w_up, w_down)


def body(
    tokens,
    memory,
    normalizer,
    stabilizer,
    norm_gain,
    w_query,
    w_key,
    w_value,
    w_outgate,
    w_input,
    w_forget,
    forget_bias,
    w_out,
    ffn_gain,
    w_gate,
    w_up,
    w_down,
    expert_ids,
    route_weights,
):
    n = lax.axis_size("ep")
    seqs, width = tokens.shape
    heads, key_size, value_size = (memory.shape[1], memory.shape[2], memory.shape[3])
    value_width = heads * value_size
    key_piece = w_query.shape[2]
    value_piece = w_value.shape[2]
    in_pre, forget_pre, projected = cell_in(
        n, tokens, norm_gain, w_input, w_forget, w_query, w_key, w_value, w_outgate
    )
    narrow = heads * key_piece
    broad = heads * value_piece

    def split(first, piece):
        part = projected[:, :, first : first + heads * piece].reshape(n, seqs, heads, piece)
        return jnp.transpose(part, (1, 2, 0, 3)).reshape(seqs, heads, n * piece).astype(jnp.float32)

    query, key_heads = split(0, key_piece), split(narrow, key_piece)
    value_heads, outgate = split(2 * narrow, value_piece), split(2 * narrow + broad, value_piece)
    log_forget = jax.nn.log_sigmoid(forget_pre + forget_bias)
    scaled = query * key_size ** (-0.5)
    stab_next = jnp.maximum(log_forget + stabilizer, in_pre)
    decay = jnp.exp(log_forget + stabilizer - stab_next)
    inweight = jnp.exp(in_pre - stab_next)
    memory_next = decay[:, :, None, None] * memory + inweight[:, :, None, None] * (
        key_heads[:, :, :, None] * value_heads[:, :, None, :]
    )
    normalizer_next = decay[:, :, None] * normalizer + inweight[:, :, None] * key_heads
    numerator = jnp.einsum("shd,shde->she", scaled, memory_next, precision=lax.Precision.HIGHEST)
    denominator = jnp.sum(scaled * normalizer_next, axis=-1)
    hidden = numerator / jnp.maximum(jnp.abs(denominator), jnp.exp(-stab_next))[:, :, None]
    hidden = (hidden * jax.nn.sigmoid(outgate)).reshape(seqs, value_width).astype(jnp.bfloat16)
    labels = jnp.arange(n, dtype=jnp.int32)
    route = jnp.sum(
        jnp.where(expert_ids[:, :, None] == labels[None, None, :], route_weights[:, :, None], 0.0), axis=1
    )
    out = ffn(n, hidden, tokens, ffn_gain, route, w_out, w_gate[0], w_up[0], w_down[0])
    return (out, memory_next, normalizer_next, stab_next)


def solution(mesh):
    return jax.shard_map(
        body,
        mesh=mesh,
        in_specs=(
            P("ep", None),
            P("ep", "tp", None, None),
            P("ep", "tp", None),
            P("ep", "tp"),
            P(),
            P(None, "tp", "ep"),
            P(None, "tp", "ep"),
            P(None, "tp", "ep"),
            P(None, "tp", "ep"),
            P(None, "tp"),
            P(None, "tp"),
            P("tp"),
            P("tp", "ep"),
            P(),
            P("ep", None, "tp"),
            P("ep", None, "tp"),
            P("ep", "tp", None),
            P("ep", None),
            P("ep", None),
        ),
        out_specs=(P("ep", None), P("ep", "tp", None, None), P("ep", "tp", None), P("ep", "tp")),
        check_vma=False,
    )
```

```python
import functools

import jax
import jax.numpy as jnp
from jax import lax
from jax.experimental import pallas as pl
from jax.experimental.pallas import tpu as pltpu
from jax.sharding import PartitionSpec as P

MESH = pl.DeviceIdType.MESH
VMEM_LIMIT = 48 * 1024 * 1024
VMEM_ALL = 67043328


def product(left, right):
    return jnp.dot(left, right, preferred_element_type=jnp.float32)


def product_nt(left, right):
    return lax.dot_general(left, right, (((1,), (1,)), ((), ())), preferred_element_type=jnp.float32)


def rms_scale(values, gain):
    return values * lax.rsqrt(jnp.mean(values * values, axis=-1, keepdims=True) + 1e-06) * gain


def remote(src, dst, send_sem, recv_sem, device):
    return pltpu.make_async_remote_copy(
        src_ref=src, dst_ref=dst, send_sem=send_sem, recv_sem=recv_sem, device_id=device, device_id_type=MESH
    )


def each(low, high, step):
    def run(at, carry):
        step(at)
        return carry

    lax.fori_loop(low, high, run, 0)


def stack_rows(pieces, dest):
    rows = pieces[0]().shape[0]
    group = max(1, 16 // rows)
    for first in range(0, len(pieces), group):
        block = jnp.concatenate([piece() for piece in pieces[first : first + group]], axis=0)
        dest[first * rows : first * rows + block.shape[0], :] = block.astype(jnp.bfloat16)


class HalfGather:
    def __init__(self, n, own, gathered, sems):
        self.n, self.own, self.gathered = n, own, gathered
        self.send, self.recv, self.relay_send, self.relay_recv = sems
        self.me, self.t = lax.axis_index("ep"), lax.axis_index("tp")

    def source(self, d):
        return lax.rem(self.me + self.n - d, self.n)

    def out(self, d):
        return remote(
            self.own.at[self.t],
            self.gathered.at[self.me, self.t],
            self.send.at[d],
            self.recv.at[d],
            (lax.rem(self.me + d, self.n), self.t),
        )

    def arrival(self, d):
        slot = self.gathered.at[self.source(d), self.t]
        return remote(self.own.at[self.t], slot, self.send.at[d], self.recv.at[d], (self.me, 1 - self.t))

    def relay(self, d, half):
        slot = self.gathered.at[self.source(d), half]
        return remote(slot, slot, self.relay_send.at[d], self.relay_recv.at[d], (self.me, 1 - self.t))

    def start(self):
        each(1, self.n, lambda d: self.out(d).start())
        self.gathered[self.me] = self.own[...]

    def finish(self):
        def pass_on(d):
            self.arrival(d).wait_recv()
            self.relay(d, self.t).start()

        each(1, self.n, pass_on)
        each(1, self.n, lambda d: self.relay(d, 1 - self.t).wait_recv())

    def drain(self):
        def step(d):
            self.out(d).wait_send()
            self.relay(d, self.t).wait_send()

        each(1, self.n, step)


class Exchange:
    def __init__(self, n, outbox, inbox, send, recv, broadcast=False):
        self.n, self.outbox, self.inbox, self.send, self.recv = n, outbox, inbox, send, recv
        self.broadcast = broadcast
        self.me, self.t = lax.axis_index("ep"), lax.axis_index("tp")

    def out(self, d):
        to = lax.rem(self.me + d, self.n)
        src = self.outbox if self.broadcast else self.outbox.at[to]
        return remote(src, self.inbox.at[self.me], self.send.at[d], self.recv.at[d], (to, self.t))

    def arrival(self, d):
        source = lax.rem(self.me + self.n - d, self.n)
        src = self.outbox if self.broadcast else self.outbox.at[source]
        return remote(src, self.inbox.at[source], self.send.at[d], self.recv.at[d], (source, self.t))

    def start(self):
        each(1, self.n, lambda d: self.out(d).start())
        self.inbox[self.me] = self.outbox[...] if self.broadcast else self.outbox[self.me]

    def finish(self):
        each(1, self.n, lambda d: self.arrival(d).wait_recv())

    def drain(self):
        each(1, self.n, lambda d: self.out(d).wait_send())


def cell_in_kernel(
    n,
    tokens_hbm, gain_hbm, win_hbm, wforget_hbm, wq_ref, wk_ref, wv_ref, wo_ref,
    inpre_ref, fpre_ref, proj_ref,
    tokens_ref, gain_ref, win_ref, wforget_ref, own, gathered, weights, rows_lo, rows_hi, outbox, inbox,
    ssem, wsem, send, recv, rsend, rrecv, xsend, xrecv,
):
    me, t = lax.axis_index("ep"), lax.axis_index("tp")
    small = [
        pltpu.make_async_copy(ref, dest, ssem.at[index])
        for index, (ref, dest) in enumerate(
            ((tokens_hbm, tokens_ref), (gain_hbm, gain_ref), (win_hbm, win_ref), (wforget_hbm, wforget_ref))
        )
    ]
    for load in small:
        load.start()
    loads, first = [], 0
    for index, ref in enumerate((wq_ref, wk_ref, wv_ref, wo_ref)):
        count = ref.shape[0]
        loads.append(pltpu.make_async_copy(ref, weights.at[pl.ds(first, count)], wsem.at[index]))
        first += count
    for load in loads:
        load.start()
    barrier = pltpu.get_barrier_semaphore()
    each(1, n, lambda d: pl.semaphore_signal(barrier, inc=1, device_id=(lax.rem(me + d, n), t), device_id_type=MESH))
    pl.semaphore_signal(barrier, inc=1, device_id=(me, 1 - t), device_id_type=MESH)

    half = own.shape[2]
    seqs = own.shape[1]
    for load in small:
        load.wait()
    normed = rms_scale(tokens_ref[...].astype(jnp.float32), gain_ref[...]).astype(jnp.bfloat16)
    own[0] = normed[:, :half]
    own[1] = normed[:, half:]
    pl.semaphore_wait(barrier, n)

    gather = HalfGather(n, own, gathered, (send, recv, rsend, rrecv))
    gather.start()
    inpre_ref[...] = product_nt(normed, win_ref[...])
    fpre_ref[...] = product_nt(normed, wforget_ref[...])
    gather.finish()
    for index, dest in enumerate((rows_lo, rows_hi)):
        stack_rows([functools.partial(lambda p, i: gathered[p, i].astype(jnp.float32), p, index) for p in range(n)], dest)
    for load in loads:
        load.wait()
    result = product_nt(rows_lo[...], weights[:, :half]) + product_nt(rows_hi[...], weights[:, half:])
    for p in range(n):
        outbox[p] = result[p * seqs : (p + 1) * seqs].astype(jnp.bfloat16)
    swap = Exchange(n, outbox, inbox, xsend, xrecv)
    swap.start()
    swap.finish()
    proj_ref[...] = inbox[...]
    gather.drain()
    swap.drain()


def ffn_kernel(
    n,
    hidden_ref, tokens_ref, gain_ref, route_ref, wout_ref, wgate_ref, wup_ref, wdown_ref,
    out_ref,
    heads_in, rows_h, wout, mixbox, mixin, resid, own, gathered, rows_lo, rows_hi,
    wgate, wup, wdown, terms, other, outbox, inbox, halves,
    wsem, hsend, hrecv, msend, mrecv, send, recv, rsend, rrecv, tsend, trecv, xsend, xrecv, osend, orecv,
):
    me, t = lax.axis_index("ep"), lax.axis_index("tp")
    loads = [
        pltpu.make_async_copy(ref, dest, wsem.at[index])
        for index, (ref, dest) in enumerate(((wout_ref, wout), (wgate_ref, wgate), (wup_ref, wup), (wdown_ref, wdown)))
    ]
    for load in loads:
        load.start()
    barrier = pltpu.get_barrier_semaphore()

    def greet(d):
        to = lax.rem(me + d, n)
        pl.semaphore_signal(barrier, inc=1, device_id=(to, t), device_id_type=MESH)
        pl.semaphore_signal(barrier, inc=1, device_id=(to, 1 - t), device_id_type=MESH)

    each(1, n, greet)
    pl.semaphore_signal(barrier, inc=1, device_id=(me, 1 - t), device_id_type=MESH)
    pl.semaphore_wait(barrier, 2 * n - 1)

    seqs, half = own.shape[1], own.shape[2]
    heads = Exchange(n, hidden_ref, heads_in, hsend, hrecv, broadcast=True)
    heads.start()
    heads.finish()
    stack_rows([functools.partial(lambda p: heads_in[p].astype(jnp.float32), p) for p in range(n)], rows_h)
    loads[0].wait()
    partial_value = product(rows_h[...], wout[...])
    for p in range(n):
        mixbox[p] = partial_value[p * seqs : (p + 1) * seqs].astype(jnp.bfloat16)

    def mix_out(d, c):
        to = lax.rem(me + d, n)
        to_t = t if c == 0 else 1 - t
        return remote(mixbox.at[to], mixin.at[t, me], msend.at[c, d], mrecv.at[c, d], (to, to_t))

    def mix_arrival(d, c):
        source = lax.rem(me + n - d, n)
        from_t = t if c == 0 else 1 - t
        return remote(mixbox.at[source], mixin.at[from_t, source], msend.at[c, d], mrecv.at[c, d], (source, 1 - t))

    each(1, n, lambda d: mix_out(d, 0).start())
    each(0, n, lambda d: mix_out(d, 1).start())
    mixin[t, me] = mixbox[me]
    each(1, n, lambda d: mix_arrival(d, 0).wait_recv())
    each(0, n, lambda d: mix_arrival(d, 1).wait_recv())
    piece = mixin.shape[3]
    for p in range(n):
        mixed = (mixin[0, p].astype(jnp.float32) + mixin[1, p].astype(jnp.float32)).astype(jnp.bfloat16)
        columns = slice(p * piece, (p + 1) * piece)
        resid[:, columns] = tokens_ref[:, columns].astype(jnp.float32) + mixed.astype(jnp.float32)
    ffn_in = rms_scale(resid[...], gain_ref[...]).astype(jnp.bfloat16)
    own[0] = ffn_in[:, :half]
    own[1] = ffn_in[:, half:]
    gather = HalfGather(n, own, gathered, (send, recv, rsend, rrecv))
    gather.start()
    gather.finish()
    for index, dest in enumerate((rows_lo, rows_hi)):
        stack_rows([functools.partial(lambda p, i: gathered[p, i].astype(jnp.float32), p, index) for p in range(n)], dest)
    loads[1].wait()
    gate = product(rows_lo[...], wgate[:half]) + product(rows_hi[...], wgate[half:])
    loads[2].wait()
    up = product(rows_lo[...], wup[:half]) + product(rows_hi[...], wup[half:])
    act = (jax.nn.silu(gate) * up).astype(jnp.bfloat16)
    loads[3].wait()
    width = min(512, half)
    across = remote(terms.at[1 - t], other, tsend, trecv, (me, 1 - t))
    for index in (1 - t, t):
        for first in range(0, half, width):
            block = product(act, wdown[:, pl.ds(pl.multiple_of(index * half + first, 128), width)])
            terms[index, :, first : first + width] = block.astype(jnp.bfloat16)
        if index is not t:
            across.start()
    across.wait_recv()
    rows = max(seqs, 16)
    for first in range(0, n * seqs, rows):
        both = terms[t, first : first + rows].astype(jnp.float32) + other[first : first + rows].astype(jnp.float32)
        for at in range(rows // seqs):
            outbox[first // seqs + at] = both[at * seqs : (at + 1) * seqs].astype(jnp.bfloat16)
    swap = Exchange(n, outbox, inbox, xsend, xrecv)
    swap.start()
    swap.finish()
    total = route_ref[:, 0:1] * inbox[0].astype(jnp.float32)
    for p in range(1, n):
        total = total + route_ref[:, p : p + 1] * inbox[p].astype(jnp.float32)
    halves[t] = total.astype(jnp.bfloat16)
    give = remote(halves.at[t], halves.at[t], osend, orecv, (me, 1 - t))
    take = remote(halves.at[1 - t], halves.at[1 - t], osend, orecv, (me, 1 - t))
    give.start()
    take.wait_recv()
    for index in range(2):
        columns = slice(index * half, (index + 1) * half)
        out_ref[:, columns] = (resid[:, columns] + halves[index].astype(jnp.float32)).astype(jnp.bfloat16)
    heads.drain()
    each(1, n, lambda d: mix_out(d, 0).wait_send())
    each(0, n, lambda d: mix_out(d, 1).wait_send())
    gather.drain()
    across.wait_send()
    swap.drain()
    give.wait_send()


def vmem_spec():
    return pl.BlockSpec(memory_space=pltpu.VMEM)


def hbm_spec():
    return pl.BlockSpec(memory_space=pltpu.MemorySpace.HBM)


def any_spec():
    return pl.BlockSpec(memory_space=pl.ANY)


def cell_in(n, tokens, gain, w_input, w_forget, w_query, w_key, w_value, w_outgate):
    seqs, width = tokens.shape
    flat = [jnp.transpose(w, (1, 2, 0)).reshape(-1, width) for w in (w_query, w_key, w_value, w_outgate)]
    columns = sum(w.shape[0] for w in flat)
    heads = w_input.shape[1]
    bf16 = jnp.bfloat16
    dma = pltpu.SemaphoreType.DMA
    return pl.pallas_call(
        functools.partial(cell_in_kernel, n),
        out_shape=(
            jax.ShapeDtypeStruct((seqs, heads), jnp.float32),
            jax.ShapeDtypeStruct((seqs, heads), jnp.float32),
            jax.ShapeDtypeStruct((n, seqs, columns), bf16),
        ),
        in_specs=[hbm_spec()] * 8,
        out_specs=(vmem_spec(),) * 3,
        scratch_shapes=[
            pltpu.VMEM((seqs, width), bf16),
            pltpu.VMEM((1, width), jnp.float32),
            pltpu.VMEM((heads, width), bf16),
            pltpu.VMEM((heads, width), bf16),
            pltpu.VMEM((2, seqs, width // 2), bf16),
            pltpu.VMEM((n, 2, seqs, width // 2), bf16),
            pltpu.VMEM((columns, width), bf16),
            pltpu.VMEM((n * seqs, width // 2), bf16),
            pltpu.VMEM((n * seqs, width // 2), bf16),
            pltpu.VMEM((n, seqs, columns), bf16),
            pltpu.VMEM((n, seqs, columns), bf16),
            dma((4,)),
            dma((4,)),
        ]
        + [dma((n,))] * 6,
        compiler_params=pltpu.CompilerParams(collective_id=0, has_side_effects=True, vmem_limit_bytes=VMEM_ALL),
        name="cell_in",
    )(tokens, gain.reshape(1, width), w_input.T, w_forget.T, *flat)


def ffn(n, hidden, tokens, gain, route, w_out, w_gate, w_up, w_down):
    seqs, width = tokens.shape
    half = width // 2
    bf16 = jnp.bfloat16
    dma = pltpu.SemaphoreType.DMA
    return pl.pallas_call(
        functools.partial(ffn_kernel, n),
        out_shape=jax.ShapeDtypeStruct((seqs, width), bf16),
        in_specs=[vmem_spec()] * 4 + [any_spec()] * 4,
        out_specs=vmem_spec(),
        scratch_shapes=[
            pltpu.VMEM((n, seqs, hidden.shape[1]), bf16),
            pltpu.VMEM((n * seqs, hidden.shape[1]), bf16),
            pltpu.VMEM(w_out.shape, bf16),
            pltpu.VMEM((n, seqs, w_out.shape[1]), bf16),
            pltpu.VMEM((2, n, seqs, w_out.shape[1]), bf16),
            pltpu.VMEM((seqs, width), jnp.float32),
            pltpu.VMEM((2, seqs, half), bf16),
            pltpu.VMEM((n, 2, seqs, half), bf16),
            pltpu.VMEM((n * seqs, half), bf16),
            pltpu.VMEM((n * seqs, half), bf16),
            pltpu.VMEM(w_gate.shape, bf16),
            pltpu.VMEM(w_up.shape, bf16),
            pltpu.VMEM(w_down.shape, bf16),
            pltpu.VMEM((2, n * seqs, half), bf16),
            pltpu.VMEM((n * seqs, half), bf16),
            pltpu.VMEM((n, seqs, half), bf16),
            pltpu.VMEM((n, seqs, half), bf16),
            pltpu.VMEM((2, seqs, half), bf16),
            dma((4,)),
            dma((n,)),
            dma((n,)),
            dma((2, n)),
            dma((2, n)),
            dma((n,)),
            dma((n,)),
            dma((n,)),
            dma((n,)),
            dma,
            dma,
            dma((n,)),
            dma((n,)),
            dma,
            dma,
        ],
        compiler_params=pltpu.CompilerParams(collective_id=1, has_side_effects=True, vmem_limit_bytes=VMEM_LIMIT),
        name="ffn",
    )(hidden, tokens, gain.reshape(1, width), route, w_out, w_gate, w_up, w_down)


def body(
    tokens,
    memory,
    normalizer,
    stabilizer,
    norm_gain,
    w_query,
    w_key,
    w_value,
    w_outgate,
    w_input,
    w_forget,
    forget_bias,
    w_out,
    ffn_gain,
    w_gate,
    w_up,
    w_down,
    expert_ids,
    route_weights,
):
    n = lax.axis_size("ep")
    seqs, width = tokens.shape
    heads, key_size, value_size = (memory.shape[1], memory.shape[2], memory.shape[3])
    value_width = heads * value_size
    key_piece = w_query.shape[2]
    value_piece = w_value.shape[2]
    in_pre, forget_pre, projected = cell_in(
        n, tokens, norm_gain, w_input, w_forget, w_query, w_key, w_value, w_outgate
    )
    narrow = heads * key_piece
    broad = heads * value_piece

    def split(first, piece):
        part = projected[:, :, first : first + heads * piece].reshape(n, seqs, heads, piece)
        return jnp.transpose(part, (1, 2, 0, 3)).reshape(seqs, heads, n * piece).astype(jnp.float32)

    query, key_heads = split(0, key_piece), split(narrow, key_piece)
    value_heads, outgate = split(2 * narrow, value_piece), split(2 * narrow + broad, value_piece)
    log_forget = jax.nn.log_sigmoid(forget_pre + forget_bias)
    scaled = query * key_size ** (-0.5)
    stab_next = jnp.maximum(log_forget + stabilizer, in_pre)
    decay = jnp.exp(log_forget + stabilizer - stab_next)
    inweight = jnp.exp(in_pre - stab_next)
    memory_next = decay[:, :, None, None] * memory + inweight[:, :, None, None] * (
        key_heads[:, :, :, None] * value_heads[:, :, None, :]
    )
    normalizer_next = decay[:, :, None] * normalizer + inweight[:, :, None] * key_heads
    numerator = jnp.einsum("shd,shde->she", scaled, memory_next, precision=lax.Precision.HIGHEST)
    denominator = jnp.sum(scaled * normalizer_next, axis=-1)
    hidden = numerator / jnp.maximum(jnp.abs(denominator), jnp.exp(-stab_next))[:, :, None]
    hidden = (hidden * jax.nn.sigmoid(outgate)).reshape(seqs, value_width).astype(jnp.bfloat16)
    labels = jnp.arange(n, dtype=jnp.int32)
    route = jnp.sum(
        jnp.where(expert_ids[:, :, None] == labels[None, None, :], route_weights[:, :, None], 0.0), axis=1
    )
    out = ffn(n, hidden, tokens, ffn_gain, route, w_out, w_gate[0], w_up[0], w_down[0])
    return (out, memory_next, normalizer_next, stab_next)


def solution(mesh):
    return jax.shard_map(
        body,
        mesh=mesh,
        in_specs=(
            P("ep", None),
            P("ep", "tp", None, None),
            P("ep", "tp", None),
            P("ep", "tp"),
            P(),
            P(None, "tp", "ep"),
            P(None, "tp", "ep"),
            P(None, "tp", "ep"),
            P(None, "tp", "ep"),
            P(None, "tp"),
            P(None, "tp"),
            P("tp"),
            P("tp", "ep"),
            P(),
            P("ep", None, "tp"),
            P("ep", None, "tp"),
            P("ep", "tp", None),
            P("ep", None),
            P("ep", None),
        ),
        out_specs=(P("ep", None), P("ep", "tp", None, None), P("ep", "tp", None), P("ep", "tp")),
        check_vma=False,
    )
```
